32 devices in a mesh: sp: 8 (over z, x), tp: 4 (over y, core).
Axes of the slice: x: 2, y: 2, z: 4, core: 2. Of those that a mesh axis runs over, the one named last changes fastest.
Arguments:
- glu_value: bfloat16 [1024, 2048], P('tp', 'sp')
- glu_gate: bfloat16 [1024, 2048], P('tp', 'sp'), may hold values from -8 to 8
- conv_taps: float32 [1024, 31], P('tp'), may hold values from -1 to 1
- norm_gain: float32 [1024], P('tp'), may hold values from 0.1 to 1.9
- out_proj: bfloat16 [1024, 2048], P(None, 'tp'), may hold values from -0.1875 to 0.1875
- resid: bfloat16 [2048, 2048], P('sp', 'tp'), may hold values from -6 to 6
- expert_ids: int32 [2048, 2], P('sp'), may hold values from 0 to 7, all different within a row; in each aligned block of 256 rows (0 to 255, 256 to 511, ...) at most 128 rows name the same one
- route_logits: float32 [2048, 2], P('sp'), may hold values from -8 to 8
- group_prob: float32 [2048], P('sp'), may hold values from 0.2 to 1
- w_gate: bfloat16 [8, 2048, 4096], P('sp', None, 'tp'), may hold values from -0.125 to 0.125
- w_up: bfloat16 [8, 2048, 4096], P('sp', None, 'tp'), may hold values from -0.125 to 0.125
- w_down: bfloat16 [8, 4096, 2048], P('sp', None, 'tp'), may hold values from -0.09375 to 0.09375
Outputs:
- layer_out: bfloat16 [2048, 2048], P('sp', 'tp')
The draws below stay inside these ranges and needn't reach their ends.
Inputs may be any that keep to these rules, and one draw needn't show every extreme that they name: `expert_ids`: each row names 2 different experts. In each aligned block of 256 rows (the rows of one index of sp) no expert is named by more than 128 rows, a bound that some block reaches.
All inputs are finite; a program needn't handle non-finite values.
Results may differ from the reference program's by a relative error of at most 0.0061.
Values may be sent and summed in bfloat16 or wider, within the bound.
A program may use at most 64 MiB of HBM per device.

```python
import math
import jax
import jax.numpy as jnp
import numpy as np
from jax import lax

D = 2048
CH = 1024
FF = 4096
KW = 31
TOPK = 2
TOK_DEV = 256
TOKENS = 2048
EXPERTS = 8
CAP = 128
N_SP = 8


def draw_glu_value(key, part):
    keyset = jax.random.split(key, 2)
    position = jnp.arange(CH, dtype=jnp.float32) / CH
    column = 10.0 ** position * jax.random.uniform(keyset[1], (CH,), jnp.float32, 0.5, 1.5)
    sample = jax.random.normal(keyset[0], (CH, TOKENS), jnp.float32)
    return (sample * column[:, None]).astype(jnp.bfloat16)


def block_scale(own_key, extent, cuts, smallest, largest):
    loudness = 1.0
    for axis_at, parts in cuts:
        steps = jax.random.uniform(jax.random.fold_in(jax.random.fold_in(own_key, 6), axis_at), (parts,), jnp.float32, smallest / len(cuts), largest / len(cuts))
        loudness = loudness * jnp.repeat(jnp.exp(steps), extent[axis_at] // parts).reshape((-1,) + (1,) * (len(extent) - 1 - axis_at))
    return loudness


def routed_block(rng, own, number, rows, amount, top, bound, slope):
    order = jax.random.permutation(rng, amount)
    packed, usual = shares(amount, rows * top, bound, slope, True), shares(amount, rows * top, bound, slope, False)
    places = jnp.arange(amount)

    def named(sizes, rotation):
        used = int((sizes > 0).sum())
        fixed = max(1, used // 4)
        passed = fixed + (places - fixed + rotation * (used - fixed)) % max(1, amount - fixed)
        return jnp.zeros((amount,), jnp.int32).at[order[jnp.where(places < fixed, places, passed)]].set(jnp.asarray(sizes, jnp.int32))

    sizes = jnp.where(number % 4 == 0, named(packed, number // 4), named(usual, number - number // 4 - 1))
    mixed = jax.random.permutation(jax.random.fold_in(own, 3), amount)
    donor, sink = mixed[0:amount // 2 * 2:2], mixed[1:amount // 2 * 2:2]
    margin = jnp.minimum(sizes[donor] - 1, bound - sizes[sink]) // 2
    margin = jnp.where((donor == order[0]) | (sink == order[0]) | (sizes[sink] == 0), 0, jnp.maximum(margin, 0))
    passed = jax.random.randint(jax.random.fold_in(own, 4), (amount // 2,), 0, 1 << 20) % (margin + 1)
    sizes = sizes.at[donor].add(-passed).at[sink].add(passed)
    members = jnp.searchsorted(jnp.cumsum(sizes), jnp.arange(rows * top), side="right").astype(jnp.int32)
    listing = members.reshape(top, rows).T
    listing = listing[jax.random.permutation(jax.random.fold_in(own, 1), rows)]
    rotation = jax.random.randint(jax.random.fold_in(own, 2), (rows, 1), 0, top)
    return jnp.take_along_axis(listing, (jnp.arange(top)[None, :] + rotation) % top, axis=1)


def shares(count, total, reach, slope, full):
    portions = [(1 << 20) // math.isqrt(rank ** slope) + 1 for rank in range(1, count + 1)]
    largest = reach if full else min(reach, max(-(-total // count), total * portions[0] // sum(portions)))
    least = 1 if total - largest >= count - 1 else 0
    holding, surplus = [largest] + [least] * (count - 1), total - largest - least * (count - 1)
    while surplus > 0:
        free = [i for i in range(1, count) if holding[i] < largest] or [i for i in range(1, count) if holding[i] < reach]
        pool, left = sum([portions[i] for i in free]), surplus
        for i in free:
            more = min(reach - holding[i], max(1, left * portions[i] // pool), surplus)
            holding[i] = holding[i] + more
            surplus = surplus - more
    return np.array(holding)


def scatter_about(rng, dims, scale, most, shards=(), kind=jnp.bfloat16):
    entries = scale * jax.random.normal(rng, dims, jnp.float32)
    if shards:
        entries = entries * block_scale(rng, dims, shards, -0.22, 0.18)
    return jnp.clip(entries, -most, most).astype(kind)


def setup_inputs(seed: int = 0) -> dict:
    key_list = jax.random.split(jax.random.key(seed), 13)
    glu_value = draw_glu_value(jax.random.fold_in(key_list[12], 71), 0)
    glu_gate = scatter_about(key_list[1], (CH, TOKENS), 1.5, 8.0, ((0, 4), (1, 8)))
    conv_taps = scatter_about(key_list[2], (CH, KW), KW ** -0.5, 1.0, ((0, 4),), jnp.float32)
    norm_gain = jnp.clip(1.0 + 0.18 * jax.random.normal(key_list[3], (CH,), jnp.float32), 0.1, 1.9)
    out_proj = scatter_about(key_list[4], (CH, D), CH ** -0.5, 0.1875, ((1, 4),))
    resid = scatter_about(key_list[5], (TOKENS, D), 1.0, 6.0, ((0, 8), (1, 4)))
    expert_ids_keys = jax.random.split(jax.random.fold_in(key_list[6], 1), TOKENS // TOK_DEV)
    expert_ids_turns = jax.random.permutation(jax.random.fold_in(key_list[6], 3), TOKENS // TOK_DEV)
    expert_ids = jax.vmap(lambda own, number: routed_block(jax.random.fold_in(key_list[6], 2), own, number, TOK_DEV, EXPERTS, TOPK, CAP, 2))(expert_ids_keys, expert_ids_turns).reshape((TOKENS, TOPK))
    route_logits = scatter_about(key_list[7], (TOKENS, TOPK), 1.5, 8.0, ((0, 8),), jnp.float32)
    group_prob = jnp.clip(jnp.exp(math.log(1.0) - 1.609438 * jax.random.uniform(key_list[8], (TOKENS,), jnp.float32) ** block_scale(key_list[8], (TOKENS,), ((0, 8),), -0.2, 0.2)), 0.2, 1.0)
    w_gate = scatter_about(key_list[9], (EXPERTS, D, FF), D ** -0.5, 0.125, ((0, 8), (2, 4)))
    w_up = scatter_about(key_list[10], (EXPERTS, D, FF), D ** -0.5, 0.125, ((0, 8), (2, 4)))
    w_down = scatter_about(key_list[11], (EXPERTS, FF, D), FF ** -0.5, 0.09375, ((0, 8), (2, 4)))
    return dict(glu_value=glu_value, glu_gate=glu_gate, conv_taps=conv_taps, norm_gain=norm_gain, out_proj=out_proj, resid=resid, expert_ids=expert_ids, route_logits=route_logits, group_prob=group_prob, w_gate=w_gate, w_up=w_up, w_down=w_down)


def reference(glu_value, glu_gate, conv_taps, norm_gain, out_proj, resid, expert_ids, route_logits, group_prob, w_gate, w_up, w_down):
    gated = (glu_value.astype(jnp.float32) * jax.nn.sigmoid(glu_gate.astype(jnp.float32))).astype(jnp.bfloat16)
    padded = jnp.pad(gated.astype(jnp.float32), ((0, 0), (KW - 1, 0)))
    filtered = jnp.zeros((CH, TOKENS), jnp.float32)
    for offset in range(KW):
        filtered = filtered + conv_taps[:, offset:offset + 1] * padded[:, offset:offset + TOKENS]
    mean = lax.optimization_barrier(jnp.sum(filtered, axis=0)) / CH
    meansq = lax.optimization_barrier(jnp.sum(filtered * filtered, axis=0)) / CH
    var = meansq - mean * mean
    normed = (filtered - mean[None, :]) * lax.rsqrt(var[None, :] + 1e-05) * norm_gain[:, None]
    activated = jax.nn.silu(normed).astype(jnp.bfloat16)
    projected = lax.dot_general(activated, out_proj, (((0,), (0,)), ((), ())), preferred_element_type=jnp.float32)
    mixed = (resid.astype(jnp.float32) + projected).astype(jnp.bfloat16)
    route_weight = group_prob[:, None] * jax.nn.softmax(route_logits, axis=-1)
    most_rows = N_SP * CAP

    def one_expert(carry, inputs):
        index, gate_mat, up_mat, down_mat = inputs
        chosen = expert_ids == index
        named = jnp.any(chosen, axis=1)
        row_index = jnp.nonzero(named, size=most_rows, fill_value=0)[0].astype(jnp.int32)
        valid = jnp.arange(most_rows) < jnp.sum(named.astype(jnp.int32))
        weight_row = lax.optimization_barrier(jnp.sum(jnp.where(chosen, route_weight, 0.0), axis=1))
        rows = jnp.take(mixed, row_index, axis=0)
        gate_part = jnp.dot(rows, gate_mat, preferred_element_type=jnp.float32)
        up_part = jnp.dot(rows, up_mat, preferred_element_type=jnp.float32)
        hidden = (jax.nn.silu(gate_part) * up_part).astype(jnp.bfloat16)
        expert_out = jnp.dot(hidden, down_mat, preferred_element_type=jnp.float32).astype(jnp.bfloat16)
        scaled = jnp.where(valid, jnp.take(weight_row, row_index), 0.0)
        carry = carry.at[row_index].add(scaled[:, None] * expert_out.astype(jnp.float32))
        return (carry, None)
    routed, _ = lax.scan(one_expert, jnp.zeros((TOKENS, D), jnp.float32), (jnp.arange(EXPERTS, dtype=jnp.int32), w_gate, w_up, w_down))
    return (mixed.astype(jnp.float32) + routed).astype(jnp.bfloat16)
```

```python
import functools

import jax
import jax.numpy as jnp
from jax import lax
from jax.experimental import pallas as pl
from jax.experimental.pallas import tpu as pltpu
from jax.sharding import PartitionSpec as P

MESH = pl.DeviceIdType.MESH


def expert_kernel(
    n_sp,
    n_tp,
    outgoing,
    w_gate,
    w_up,
    w_down,
    returned,
    rows,
    hidden,
    results,
    gate_v,
    up_v,
    down_v,
    load_sem,
    own_sem,
    out_send,
    rows_recv,
    rows_far,
    rows_near,
    hid_recv,
    hid_far,
    hid_near,
    ret_send,
    ret_recv,
):
    e = lax.axis_index("sp")
    q = lax.axis_index("tp")
    n_y = n_tp // 2
    y, core = q // 2, q % 2
    sibling = 2 * y + (1 - core)
    width = outgoing.shape[2]
    ff_local = gate_v.shape[1]

    def source(k):
        return lax.rem(e + k, n_sp)

    def rows_at(s, t):
        return rows.at[s, :, pl.ds(pl.multiple_of(t * width, width), width)]

    def hidden_at(s, t):
        return hidden.at[s, :, pl.ds(pl.multiple_of(t * ff_local, ff_local), ff_local)]

    def far(j):
        return 2 * lax.rem(y + j, n_y) + core

    def behind(j):
        return 2 * lax.rem(y + n_y - j, n_y) + core

    def share(at, recv, s, t, send, peer):
        return pltpu.make_async_remote_copy(
            src_ref=at(s, t),
            dst_ref=at(s, t),
            send_sem=send,
            recv_sem=recv.at[s, t],
            device_id=(e, peer),
            device_id_type=MESH,
        )

    def dispatch(k):
        to = lax.rem(e + n_sp - k, n_sp)
        return pltpu.make_async_remote_copy(
            src_ref=outgoing.at[to],
            dst_ref=rows_at(e, q),
            send_sem=out_send.at[k],
            recv_sem=rows_recv.at[e, q],
            device_id=(to, q),
            device_id_type=MESH,
        )

    def give_back(k):
        s = source(k)
        return pltpu.make_async_remote_copy(
            src_ref=results.at[s],
            dst_ref=returned.at[e],
            send_sem=ret_send.at[k],
            recv_sem=ret_recv.at[e],
            device_id=(s, q),
            device_id_type=MESH,
        )

    def arrived(at, recv, s, t):
        pltpu.make_async_copy(at(s, t), at(s, t), recv.at[s, t]).wait()

    loads = [
        pltpu.make_async_copy(w_gate.at[0], gate_v, load_sem.at[0]),
        pltpu.make_async_copy(w_up.at[0], up_v, load_sem.at[1]),
        pltpu.make_async_copy(w_down.at[0], down_v, load_sem.at[2]),
    ]
    own_in = pltpu.make_async_copy(outgoing.at[e], rows_at(e, q), own_sem.at[0])
    own_in.start()

    barrier = pltpu.get_barrier_semaphore()

    @pl.loop(1, n_sp)
    def _(k):
        pl.semaphore_signal(barrier, inc=1, device_id=(source(k), q), device_id_type=MESH)

    for j in range(1, n_y):
        pl.semaphore_signal(barrier, inc=1, device_id=(e, far(j)), device_id_type=MESH)
    pl.semaphore_signal(barrier, inc=1, device_id=(e, sibling), device_id_type=MESH)
    pl.semaphore_wait(barrier, n_sp - 1 + n_y)

    @pl.loop(1, n_sp)
    def _(k):
        dispatch(k).start()

    for load in loads:
        load.start()

    def spread(at, recv, far_sem, near_sem, s):
        for j in range(1, n_y):
            share(at, recv, s, q, far_sem.at[s, j], far(j)).start()
        share(at, recv, s, q, near_sem.at[s, 0], sibling).start()

    def relay(at, recv, near_sem, s):
        for j in range(1, n_y):
            t = behind(j)
            arrived(at, recv, s, t)
            share(at, recv, s, t, near_sem.at[s, j], sibling).start()

    def collect(at, recv, s):
        for j in range(n_y):
            arrived(at, recv, s, 2 * lax.rem(y + n_y - j, n_y) + (1 - core))

    def drain(at, recv, far_sem, near_sem, s):
        for j in range(1, n_y):
            share(at, recv, s, q, far_sem.at[s, j], far(j)).wait_send()
        share(at, recv, s, q, near_sem.at[s, 0], sibling).wait_send()
        for j in range(1, n_y):
            share(at, recv, s, behind(j), near_sem.at[s, j], sibling).wait_send()

    tile = min(256, ff_local)
    out_tile = min(256, width)

    def up_step(s):
        @pl.loop(0, ff_local // tile)
        def _(i):
            at = pl.ds(pl.multiple_of(i * tile, tile), tile)
            g = jnp.dot(rows[s], gate_v[:, at], preferred_element_type=jnp.float32)
            u = jnp.dot(rows[s], up_v[:, at], preferred_element_type=jnp.float32)
            h = (g / (1.0 + jnp.exp(-g)) * u).astype(hidden.dtype)
            hidden[s, :, pl.ds(pl.multiple_of(q * ff_local + i * tile, tile), tile)] = h

    def down_step(s):
        @pl.loop(0, width // out_tile)
        def _(i):
            at = pl.ds(pl.multiple_of(i * out_tile, out_tile), out_tile)
            o = jnp.dot(hidden[s], down_v[:, at], preferred_element_type=jnp.float32)
            results[s, :, at] = o.astype(results.dtype)

    @pl.loop(0, n_sp + 4)
    def _(i):
        @pl.when(i < n_sp)
        def _():
            @pl.when(i == 0)
            def _():
                own_in.wait()

            @pl.when(i > 0)
            def _():
                arrived(rows_at, rows_recv, source(i), q)

            spread(rows_at, rows_recv, rows_far, rows_near, source(i))

        @pl.when((i >= 1) & (i < n_sp + 1))
        def _():
            relay(rows_at, rows_recv, rows_near, source(i - 1))

        @pl.when((i >= 2) & (i < n_sp + 2))
        def _():
            s = source(i - 2)
            collect(rows_at, rows_recv, s)

            @pl.when(i == 2)
            def _():
                for load in loads:
                    load.wait()

            up_step(s)
            spread(hidden_at, hid_recv, hid_far, hid_near, s)

        @pl.when((i >= 3) & (i < n_sp + 3))
        def _():
            relay(hidden_at, hid_recv, hid_near, source(i - 3))

        @pl.when(i >= 4)
        def _():
            s = source(i - 4)
            collect(hidden_at, hid_recv, s)
            down_step(s)

            @pl.when(i == 4)
            def _():
                pltpu.make_async_copy(results.at[e], returned.at[e], own_sem.at[1]).start()

            @pl.when(i > 4)
            def _():
                give_back(i - 4).start()

    pltpu.make_async_copy(results.at[e], returned.at[e], own_sem.at[1]).wait()

    @pl.loop(0, n_sp)
    def _(s):
        drain(rows_at, rows_recv, rows_far, rows_near, s)
        drain(hidden_at, hid_recv, hid_far, hid_near, s)

    @pl.loop(1, n_sp)
    def _(k):
        dispatch(k).wait_send()
        give_back(k).wait_send()
        s = source(k)
        pltpu.make_async_copy(returned.at[s], returned.at[s], ret_recv.at[s]).wait()


def run_experts(outgoing, w_gate, w_up, w_down):
    n_sp, n_tp = lax.axis_size("sp"), lax.axis_size("tp")
    n_y = n_tp // 2
    _, capacity, width = outgoing.shape
    ff_local = w_gate.shape[2]
    dma = pltpu.SemaphoreType.DMA
    return pl.pallas_call(
        functools.partial(expert_kernel, n_sp, n_tp),
        out_shape=jax.ShapeDtypeStruct(outgoing.shape, outgoing.dtype),
        in_specs=[pl.BlockSpec(memory_space=pl.ANY)] * 4,
        out_specs=pl.BlockSpec(memory_space=pl.ANY),
        scratch_shapes=[
            pltpu.VMEM((n_sp, capacity, width * n_tp), jnp.bfloat16),
            pltpu.VMEM((n_sp, capacity, ff_local * n_tp), jnp.bfloat16),
            pltpu.VMEM(outgoing.shape, jnp.bfloat16),
            pltpu.VMEM(w_gate.shape[1:], jnp.bfloat16),
            pltpu.VMEM(w_up.shape[1:], jnp.bfloat16),
            pltpu.VMEM(w_down.shape[1:], jnp.bfloat16),
            dma((3,)),
            dma((2,)),
            dma((n_sp,)),
            dma((n_sp, n_tp)),
            dma((n_sp, n_y)),
            dma((n_sp, n_y)),
            dma((n_sp, n_tp)),
            dma((n_sp, n_y)),
            dma((n_sp, n_y)),
            dma((n_sp,)),
            dma((n_sp,)),
        ],
        compiler_params=pltpu.CompilerParams(
            collective_id=0, has_side_effects=True, vmem_limit_bytes=48 * 1024 * 1024
        ),
    )(outgoing, w_gate, w_up, w_down)


def from_behind(block, axis, distance):
    devices = range(lax.axis_size(axis))
    route = [(i - distance, i) for i in devices if i - distance in devices]
    return lax.ppermute(block, axis, route)


def per_device(
    glu_value,
    glu_gate,
    conv_taps,
    norm_gain,
    out_proj,
    resid,
    expert_ids,
    route_logits,
    group_prob,
    w_gate,
    w_up,
    w_down,
):
    local_tokens = glu_value.shape[1]
    tap_count = conv_taps.shape[1]
    channels = glu_value.shape[0] * lax.axis_size("tp")
    gated = (glu_value.astype(jnp.float32) * jax.nn.sigmoid(glu_gate.astype(jnp.float32))).astype(
        jnp.bfloat16
    )
    history = from_behind(gated[:, local_tokens - (tap_count - 1) :], "sp", 1)
    padded = jnp.concatenate([history, gated], axis=1).astype(jnp.float32)
    filtered = jnp.zeros(gated.shape, jnp.float32)
    for offset in range(tap_count):
        filtered = (
            filtered + conv_taps[:, offset : offset + 1] * padded[:, offset : offset + local_tokens]
        )
    total_one, total_two = lax.psum(
        (jnp.sum(filtered, axis=0), jnp.sum(filtered * filtered, axis=0)), "tp"
    )
    mean = total_one / channels
    var = total_two / channels - mean * mean
    normed = (filtered - mean[None, :]) * lax.rsqrt(var[None, :] + 1e-05) * norm_gain[:, None]
    activated = jax.nn.silu(normed).astype(jnp.bfloat16)
    weights = out_proj
    projected = lax.dot_general(
        lax.all_gather(activated, "tp", axis=0, tiled=True),
        weights,
        (((0,), (0,)), ((), ())),
        preferred_element_type=jnp.float32,
    )
    mixed = (resid.astype(jnp.float32) + projected).astype(jnp.bfloat16)
    experts = lax.axis_size("sp")
    capacity = 4 * local_tokens // experts
    flat_ids = expert_ids.reshape(-1)
    onehot = (flat_ids[:, None] == jnp.arange(experts, dtype=jnp.int32)[None, :]).astype(jnp.int32)
    rank = jnp.sum(jnp.cumsum(onehot, axis=0) * onehot, axis=1) - 1
    slot = flat_ids * capacity + rank
    token_of = jnp.arange(flat_ids.shape[0], dtype=jnp.int32) // expert_ids.shape[1]
    table = jnp.zeros((experts * capacity,), jnp.int32).at[slot].set(token_of)
    route_weight = (group_prob[:, None] * jax.nn.softmax(route_logits, axis=-1)).reshape(-1)
    outgoing = jnp.take(mixed, table, axis=0).reshape(experts, capacity, mixed.shape[1])
    returned = run_experts(outgoing, w_gate, w_up, w_down)
    flat_back = returned.reshape(experts * capacity, returned.shape[2])
    picked = jnp.take(flat_back, slot, axis=0).astype(jnp.float32) * route_weight[:, None]
    routed = jnp.sum(picked.reshape(local_tokens, expert_ids.shape[1], flat_back.shape[1]), axis=1)
    return (mixed.astype(jnp.float32) + routed).astype(jnp.bfloat16)


def solution(mesh):
    return jax.shard_map(
        per_device,
        mesh=mesh,
        in_specs=(
            P("tp", "sp"),
            P("tp", "sp"),
            P("tp", None),
            P("tp"),
            P(None, "tp"),
            P("sp", "tp"),
            P("sp", None),
            P("sp", None),
            P("sp"),
            P("sp", None, "tp"),
            P("sp", None, "tp"),
            P("sp", None, "tp"),
        ),
        out_specs=P("sp", "tp"),
        check_vma=False,
    )
```

```python
import functools

import jax
import jax.numpy as jnp
from jax import lax
from jax.experimental import pallas as pl
from jax.experimental.pallas import tpu as pltpu
from jax.sharding import PartitionSpec as P

MESH = pl.DeviceIdType.MESH


def expert_kernel(
    n_sp,
    n_tp,
    filtered,
    gain,
    proj,
    resid,
    slot_rows,
    slot_cols,
    route,
    w_gate,
    w_up,
    w_down,
    out,
    stats,
    act,
    mixed,
    total,
    outgoing,
    rows,
    hidden,
    results,
    returned,
    gate_v,
    up_v,
    down_v,
    load_sem,
    own_sem,
    stat_send,
    stat_recv,
    act_recv,
    act_far,
    act_near,
    mix_send,
    mix_recv,
    out_send,
    rows_recv,
    rows_near,
    hid_recv,
    hid_far,
    hid_near,
    ret_send,
    ret_recv,
):
    e = lax.axis_index("sp")
    q = lax.axis_index("tp")
    n_y = n_tp // 2
    y, core = q // 2, q % 2
    sibling = 2 * y + (1 - core)
    _, capacity, width = results.shape
    wide = n_y * width
    tokens = mixed.shape[0]
    ff_local = gate_v.shape[1]

    def source(k):
        return lax.rem(e + k, n_sp)

    def rows_at(s, c):
        return rows.at[s, :, pl.ds(pl.multiple_of(c * wide, wide), wide)]

    def act_at(s, t):
        return act.at[t]

    def mixed_at(t):
        return mixed.at[:, pl.ds(pl.multiple_of((t // 2) * width, width), width)]

    def hidden_at(s, t):
        return hidden.at[s, :, pl.ds(pl.multiple_of(t * ff_local, ff_local), ff_local)]

    def far(j):
        return 2 * lax.rem(y + j, n_y) + core

    def behind(j):
        return 2 * lax.rem(y + n_y - j, n_y) + core

    def share(at, recv, s, t, send, peer):
        return pltpu.make_async_remote_copy(
            src_ref=at(s, t),
            dst_ref=at(s, t),
            send_sem=send,
            recv_sem=recv.at[s, t],
            device_id=(e, peer),
            device_id_type=MESH,
        )

    def dispatch(k):
        to = lax.rem(e + n_sp - k, n_sp)
        return pltpu.make_async_remote_copy(
            src_ref=outgoing.at[to],
            dst_ref=rows_at(e, core),
            send_sem=out_send.at[k],
            recv_sem=rows_recv.at[e, core],
            device_id=(to, q),
            device_id_type=MESH,
        )

    def give_back(k):
        s = source(k)
        return pltpu.make_async_remote_copy(
            src_ref=results.at[s],
            dst_ref=returned.at[e],
            send_sem=ret_send.at[k],
            recv_sem=ret_recv.at[e],
            device_id=(s, q),
            device_id_type=MESH,
        )

    def arrived(at, recv, s, t):
        pltpu.make_async_copy(at(s, t), at(s, t), recv.at[s, t]).wait()

    def tell(o):
        return pltpu.make_async_remote_copy(
            src_ref=stats.at[q],
            dst_ref=stats.at[q],
            send_sem=stat_send.at[o],
            recv_sem=stat_recv.at[q],
            device_id=(e, lax.rem(q + o, n_tp)),
            device_id_type=MESH,
        )

    def cross(j):
        return pltpu.make_async_remote_copy(
            src_ref=mixed_at(q),
            dst_ref=mixed_at(q),
            send_sem=mix_send.at[j],
            recv_sem=mix_recv.at[y],
            device_id=(e, far(j)),
            device_id_type=MESH,
        )

    loads = [pltpu.make_async_copy(w_down.at[0], down_v, load_sem.at[2, 0])]
    for t in range(n_tp):
        to = pl.ds((t % 2 * n_y + t // 2) * width, width)
        at = pl.ds(t * width, width)
        loads.append(pltpu.make_async_copy(w_gate.at[0, at], gate_v.at[to], load_sem.at[0, t]))
        loads.append(pltpu.make_async_copy(w_up.at[0, at], up_v.at[to], load_sem.at[1, t]))

    barrier = pltpu.get_barrier_semaphore()

    @pl.loop(1, n_sp)
    def _(k):
        pl.semaphore_signal(barrier, inc=1, device_id=(source(k), q), device_id_type=MESH)

    for o in range(1, n_tp):
        pl.semaphore_signal(
            barrier, inc=1, device_id=(e, lax.rem(q + o, n_tp)), device_id_type=MESH
        )
    for load in loads:
        load.start()

    raw = filtered[...]
    stats[q, 0:1] = jnp.sum(raw, axis=0, keepdims=True)
    stats[q, 1:2] = jnp.sum(raw * raw, axis=0, keepdims=True)
    pl.semaphore_wait(barrier, n_sp - 1 + n_tp - 1)

    def spread(at, recv, far_sem, near_sem, s):
        for j in range(1, n_y):
            share(at, recv, s, q, far_sem.at[s, j], far(j)).start()
        share(at, recv, s, q, near_sem.at[s, 0], sibling).start()

    def relay(at, recv, near_sem, s):
        for j in range(1, n_y):
            t = behind(j)
            arrived(at, recv, s, t)
            share(at, recv, s, t, near_sem.at[s, j], sibling).start()

    def collect(at, recv, s):
        for j in range(n_y):
            arrived(at, recv, s, 2 * lax.rem(y + n_y - j, n_y) + (1 - core))

    def drain(at, recv, far_sem, near_sem, s):
        for j in range(1, n_y):
            share(at, recv, s, q, far_sem.at[s, j], far(j)).wait_send()
        share(at, recv, s, q, near_sem.at[s, 0], sibling).wait_send()
        for j in range(1, n_y):
            share(at, recv, s, behind(j), near_sem.at[s, j], sibling).wait_send()

    for o in range(1, n_tp):
        tell(o).start()
    for o in range(1, n_tp):
        t = lax.rem(q + o, n_tp)
        pltpu.make_async_copy(stats.at[t], stats.at[t], stat_recv.at[t]).wait()
    one = stats[0, 0:1]
    two = stats[0, 1:2]
    for t in range(1, n_tp):
        one = one + stats[t, 0:1]
        two = two + stats[t, 1:2]
    channels = proj.shape[0]
    mean = one / channels
    var = two / channels - mean * mean
    normed = (filtered[...] - mean) * lax.rsqrt(var + 1e-05) * gain[...]
    act[q] = (normed / (1.0 + jnp.exp(-normed))).astype(act.dtype)
    spread(act_at, act_recv, act_far, act_near, 0)
    relay(act_at, act_recv, act_near, 0)
    collect(act_at, act_recv, 0)
    depth = act.shape[1]
    sums = resid[...].astype(jnp.float32)
    for t in range(n_tp):
        sums = sums + lax.dot_general(
            act[t],
            proj[t * depth : (t + 1) * depth],
            (((0,), (0,)), ((), ())),
            preferred_element_type=jnp.float32,
        )
    own_columns = pl.ds(pl.multiple_of(y * width, width), width)
    mixed[:, own_columns] = sums.astype(mixed.dtype)
    for j in range(1, n_y):
        cross(j).start()
    total[...] = jnp.zeros_like(total)
    for j in range(1, n_y):
        t = behind(j)
        pltpu.make_async_copy(mixed_at(t), mixed_at(t), mix_recv.at[t // 2]).wait()

    @pl.loop(0, n_sp)
    def _(k):
        to = lax.rem(e + n_sp - k, n_sp)
        place = to * capacity + lax.broadcasted_iota(jnp.int32, (capacity, tokens), 0)
        named = place == slot_rows[0:1]
        for r in range(1, slot_rows.shape[0]):
            named = named | (place == slot_rows[r : r + 1])
        picks = jnp.where(named, 1.0, 0.0).astype(mixed.dtype)
        outgoing[to] = jnp.dot(picks, mixed[...], preferred_element_type=jnp.float32).astype(
            outgoing.dtype
        )

        @pl.when(k > 0)
        def _():
            dispatch(k).start()

    own_in = pltpu.make_async_copy(outgoing.at[e], rows_at(e, core), own_sem.at[0])
    own_in.start()

    def near_rows(s):
        return pltpu.make_async_remote_copy(
            src_ref=rows_at(s, core),
            dst_ref=rows_at(s, core),
            send_sem=rows_near.at[s],
            recv_sem=rows_recv.at[s, core],
            device_id=(e, sibling),
            device_id_type=MESH,
        )

    def combine(x):
        for r in range(slot_cols.shape[1]):
            place = x * capacity + lax.broadcasted_iota(jnp.int32, (tokens, capacity), 1)
            picks = jnp.where(place == slot_cols[:, r : r + 1], 1.0, 0.0).astype(mixed.dtype)
            got = jnp.dot(picks, returned[x], preferred_element_type=jnp.float32)
            total[...] += route[:, r : r + 1] * got

    tile = min(256, ff_local)
    out_tile = min(256, width)

    def up_step(s):
        @pl.loop(0, ff_local // tile)
        def _(i):
            at = pl.ds(pl.multiple_of(i * tile, tile), tile)
            g = jnp.dot(rows[s], gate_v[:, at], preferred_element_type=jnp.float32)
            u = jnp.dot(rows[s], up_v[:, at], preferred_element_type=jnp.float32)
            h = (g / (1.0 + jnp.exp(-g)) * u).astype(hidden.dtype)
            hidden[s, :, pl.ds(pl.multiple_of(q * ff_local + i * tile, tile), tile)] = h

    def down_step(s):
        @pl.loop(0, width // out_tile)
        def _(i):
            at = pl.ds(pl.multiple_of(i * out_tile, out_tile), out_tile)
            o = jnp.dot(hidden[s], down_v[:, at], preferred_element_type=jnp.float32)
            results[s, :, at] = o.astype(results.dtype)

    @pl.loop(0, n_sp + 3)
    def _(i):
        @pl.when(i < n_sp)
        def _():
            @pl.when(i == 0)
            def _():
                own_in.wait()

            @pl.when(i > 0)
            def _():
                arrived(rows_at, rows_recv, source(i), core)

            near_rows(source(i)).start()

        @pl.when((i >= 1) & (i < n_sp + 1))
        def _():
            s = source(i - 1)
            arrived(rows_at, rows_recv, s, 1 - core)

            @pl.when(i == 1)
            def _():
                for load in loads:
                    load.wait()

            up_step(s)
            spread(hidden_at, hid_recv, hid_far, hid_near, s)

        @pl.when((i >= 2) & (i < n_sp + 2))
        def _():
            relay(hidden_at, hid_recv, hid_near, source(i - 2))

        @pl.when(i >= 3)
        def _():
            s = source(i - 3)
            collect(hidden_at, hid_recv, s)
            down_step(s)

            @pl.when(i == 3)
            def _():
                pltpu.make_async_copy(results.at[e], returned.at[e], own_sem.at[1]).start()

            @pl.when(i > 3)
            def _():
                give_back(i - 3).start()

    pltpu.make_async_copy(results.at[e], returned.at[e], own_sem.at[1]).wait()
    combine(e)

    @pl.loop(1, n_sp)
    def _(k):
        x = lax.rem(e + n_sp - k, n_sp)
        pltpu.make_async_copy(returned.at[x], returned.at[x], ret_recv.at[x]).wait()
        combine(x)

    out[...] = (mixed[:, own_columns].astype(jnp.float32) + total[...]).astype(out.dtype)

    for o in range(1, n_tp):
        tell(o).wait_send()
    for j in range(1, n_y):
        cross(j).wait_send()
    drain(act_at, act_recv, act_far, act_near, 0)

    @pl.loop(0, n_sp)
    def _(s):
        near_rows(s).wait_send()
        drain(hidden_at, hid_recv, hid_far, hid_near, s)

    @pl.loop(1, n_sp)
    def _(k):
        dispatch(k).wait_send()
        give_back(k).wait_send()


def run_layer(filtered, gain, proj, resid, slot_rows, slot_cols, route, w_gate, w_up, w_down):
    n_sp, n_tp = lax.axis_size("sp"), lax.axis_size("tp")
    n_y = n_tp // 2
    tokens, width = resid.shape
    capacity = 4 * tokens // n_sp
    ff_local = w_gate.shape[2]
    dma = pltpu.SemaphoreType.DMA
    vmem = pl.BlockSpec(memory_space=pltpu.VMEM)
    return pl.pallas_call(
        functools.partial(expert_kernel, n_sp, n_tp),
        out_shape=jax.ShapeDtypeStruct(resid.shape, resid.dtype),
        in_specs=[vmem] * 7 + [pl.BlockSpec(memory_space=pl.ANY)] * 3,
        out_specs=vmem,
        scratch_shapes=[
            pltpu.VMEM((n_tp, 8, tokens), jnp.float32),
            pltpu.VMEM((n_tp,) + filtered.shape, jnp.bfloat16),
            pltpu.VMEM((tokens, n_y * width), jnp.bfloat16),
            pltpu.VMEM((tokens, width), jnp.float32),
            pltpu.VMEM((n_sp, capacity, n_y * width), jnp.bfloat16),
            pltpu.VMEM((n_sp, capacity, width * n_tp), jnp.bfloat16),
            pltpu.VMEM((n_sp, capacity, ff_local * n_tp), jnp.bfloat16),
            pltpu.VMEM((n_sp, capacity, width), jnp.bfloat16),
            pltpu.VMEM((n_sp, capacity, width), jnp.bfloat16),
            pltpu.VMEM(w_gate.shape[1:], jnp.bfloat16),
            pltpu.VMEM(w_up.shape[1:], jnp.bfloat16),
            pltpu.VMEM(w_down.shape[1:], jnp.bfloat16),
            dma((3, n_tp)),
            dma((2,)),
            dma((n_tp,)),
            dma((n_tp,)),
            dma((1, n_tp)),
            dma((1, n_y)),
            dma((1, n_y)),
            dma((n_y,)),
            dma((n_y,)),
            dma((n_sp,)),
            dma((n_sp, 2)),
            dma((n_sp,)),
            dma((n_sp, n_tp)),
            dma((n_sp, n_y)),
            dma((n_sp, n_y)),
            dma((n_sp,)),
            dma((n_sp,)),
        ],
        compiler_params=pltpu.CompilerParams(
            collective_id=0, has_side_effects=True, vmem_limit_bytes=52 * 1024 * 1024
        ),
    )(filtered, gain, proj, resid, slot_rows, slot_cols, route, w_gate, w_up, w_down)


def from_behind(block, axis, distance):
    devices = range(lax.axis_size(axis))
    route = [(i - distance, i) for i in devices if i - distance in devices]
    return lax.ppermute(block, axis, route)


def per_device(
    glu_value,
    glu_gate,
    conv_taps,
    norm_gain,
    out_proj,
    resid,
    expert_ids,
    route_logits,
    group_prob,
    w_gate,
    w_up,
    w_down,
):
    local_tokens = glu_value.shape[1]
    tap_count = conv_taps.shape[1]
    gated = (glu_value.astype(jnp.float32) * jax.nn.sigmoid(glu_gate.astype(jnp.float32))).astype(
        jnp.bfloat16
    )
    history = from_behind(gated[:, local_tokens - (tap_count - 1) :], "sp", 1)
    padded = jnp.concatenate([history, gated], axis=1).astype(jnp.float32)
    filtered = jnp.zeros(gated.shape, jnp.float32)
    for offset in range(tap_count):
        filtered = (
            filtered + conv_taps[:, offset : offset + 1] * padded[:, offset : offset + local_tokens]
        )
    experts = lax.axis_size("sp")
    capacity = 4 * local_tokens // experts
    flat_ids = expert_ids.reshape(-1)
    onehot = (flat_ids[:, None] == jnp.arange(experts, dtype=jnp.int32)[None, :]).astype(jnp.int32)
    rank = jnp.sum(jnp.cumsum(onehot, axis=0) * onehot, axis=1) - 1
    slot = flat_ids * capacity + rank
    slots = slot.reshape(expert_ids.shape)
    route_weight = group_prob[:, None] * jax.nn.softmax(route_logits, axis=-1)
    return run_layer(
        filtered,
        norm_gain[:, None],
        out_proj,
        resid,
        slots.T,
        slots,
        route_weight,
        w_gate,
        w_up,
        w_down,
    )


def solution(mesh):
    return jax.shard_map(
        per_device,
        mesh=mesh,
        in_specs=(
            P("tp", "sp"),
            P("tp", "sp"),
            P("tp", None),
            P("tp"),
            P(None, "tp"),
            P("sp", "tp"),
            P("sp", None),
            P("sp", None),
            P("sp"),
            P("sp", None, "tp"),
            P("sp", None, "tp"),
            P("sp", None, "tp"),
        ),
        out_specs=P("sp", "tp"),
        check_vma=False,
    )
```

```python
import functools

import jax
import jax.numpy as jnp
from jax import lax
from jax.experimental import pallas as pl
from jax.experimental.pallas import tpu as pltpu
from jax.sharding import PartitionSpec as P

MESH = pl.DeviceIdType.MESH


def expert_kernel(
    n_sp,
    n_tp,
    filtered,
    gain,
    proj,
    resid,
    id_rows,
    id_cols,
    logits,
    prob,
    w_gate,
    w_up,
    w_down,
    out,
    stats,
    act,
    mixed,
    slots,
    route,
    total,
    outgoing,
    rows,
    hidden,
    results,
    returned,
    gate_v,
    up_v,
    down_v,
    load_sem,
    own_sem,
    stat_send,
    stat_recv,
    act_recv,
    act_far,
    act_near,
    out_send,
    rows_recv,
    rows_far,
    rows_near,
    hid_recv,
    hid_far,
    hid_near,
    ret_send,
    ret_recv,
):
    e = lax.axis_index("sp")
    q = lax.axis_index("tp")
    n_y = n_tp // 2
    y, core = q // 2, q % 2
    sibling = 2 * y + (1 - core)
    _, capacity, width = results.shape
    tokens = mixed.shape[0]
    ff_local = gate_v.shape[1]

    def source(k):
        if n_sp & (n_sp - 1) or n_sp == 1:
            return lax.rem(e + k, n_sp)
        k = jnp.where(k == 0, 0, lax.rem(k, n_sp - 1) + 1) if n_sp > 2 else k
        at, bit = 0, 1
        while bit < n_sp:
            at, bit = at + (e // bit + k // bit) % 2 * bit, 2 * bit
        return at

    def target(k):
        if n_sp & (n_sp - 1) or n_sp == 1:
            return lax.rem(e + n_sp - k, n_sp)
        return source(k)

    def rows_at(s, t):
        return rows.at[s, :, pl.ds(pl.multiple_of(t * width, width), width)]

    def act_at(s, t):
        return act.at[t]

    def hidden_at(s, t):
        return hidden.at[s, :, pl.ds(pl.multiple_of(t * ff_local, ff_local), ff_local)]

    def far(j):
        return 2 * lax.rem(y + j, n_y) + core

    def behind(j):
        return 2 * lax.rem(y + n_y - j, n_y) + core

    def share(at, recv, s, t, send, peer):
        return pltpu.make_async_remote_copy(
            src_ref=at(s, t),
            dst_ref=at(s, t),
            send_sem=send,
            recv_sem=recv.at[s, t],
            device_id=(e, peer),
            device_id_type=MESH,
        )

    def dispatch(k):
        to = target(k)
        return pltpu.make_async_remote_copy(
            src_ref=outgoing.at[to],
            dst_ref=rows_at(e, q),
            send_sem=out_send.at[k],
            recv_sem=rows_recv.at[e, q],
            device_id=(to, q),
            device_id_type=MESH,
        )

    def give_back(k):
        s = source(k)
        return pltpu.make_async_remote_copy(
            src_ref=results.at[s],
            dst_ref=returned.at[e],
            send_sem=ret_send.at[k],
            recv_sem=ret_recv.at[e],
            device_id=(s, q),
            device_id_type=MESH,
        )

    def arrived(at, recv, s, t):
        pltpu.make_async_copy(at(s, t), at(s, t), recv.at[s, t]).wait()

    def tell(o):
        return pltpu.make_async_remote_copy(
            src_ref=stats.at[q],
            dst_ref=stats.at[q],
            send_sem=stat_send.at[o],
            recv_sem=stat_recv.at[q],
            device_id=(e, lax.rem(q + o, n_tp)),
            device_id_type=MESH,
        )

    loads = [
        pltpu.make_async_copy(w_gate.at[0], gate_v, load_sem.at[0]),
        pltpu.make_async_copy(w_up.at[0], up_v, load_sem.at[1]),
        pltpu.make_async_copy(w_down.at[0], down_v, load_sem.at[2]),
    ]
    barrier = pltpu.get_barrier_semaphore()

    @pl.loop(1, n_sp)
    def _(k):
        pl.semaphore_signal(barrier, inc=1, device_id=(source(k), q), device_id_type=MESH)

    for o in range(1, n_tp):
        pl.semaphore_signal(
            barrier, inc=1, device_id=(e, lax.rem(q + o, n_tp)), device_id_type=MESH
        )
    for load in loads:
        load.start()

    top = id_rows.shape[0]
    ahead = lax.broadcasted_iota(jnp.int32, (tokens, tokens), 0)
    after = lax.broadcasted_iota(jnp.int32, (tokens, tokens), 1)
    lanes = max(128, n_sp)
    row_no = lax.broadcasted_iota(jnp.int32, (lanes, tokens), 0)
    col_no = lax.broadcasted_iota(jnp.int32, (tokens, lanes), 1)
    row_hit = [jnp.where(row_no == id_rows[r : r + 1], 1.0, 0.0) for r in range(top)]
    col_hit = [jnp.where(col_no == id_cols[:, r : r + 1], 1.0, 0.0) for r in range(top)]
    row_rank = jnp.dot(
        sum(row_hit).astype(jnp.bfloat16),
        jnp.where(ahead < after, 1.0, 0.0).astype(jnp.bfloat16),
        preferred_element_type=jnp.float32,
    )
    col_rank = jnp.dot(
        jnp.where(ahead > after, 1.0, 0.0).astype(jnp.bfloat16),
        sum(col_hit).astype(jnp.bfloat16),
        preferred_element_type=jnp.float32,
    )
    slot_rows = [
        (id_rows[r : r + 1] * capacity).astype(jnp.float32)
        + jnp.sum(row_hit[r] * row_rank, axis=0, keepdims=True)
        for r in range(top)
    ]
    for r in range(top):
        slots[:, r : r + 1] = (id_cols[:, r : r + 1] * capacity).astype(jnp.float32) + jnp.sum(
            col_hit[r] * col_rank, axis=1, keepdims=True
        )
    scores = logits[...]
    scores = jnp.exp(scores - jnp.max(scores, axis=1, keepdims=True))
    route[...] = prob[...] * scores / jnp.sum(scores, axis=1, keepdims=True)
    raw = filtered[...]
    stats[q, 0:1] = jnp.sum(raw, axis=0, keepdims=True)
    stats[q, 1:2] = jnp.sum(raw * raw, axis=0, keepdims=True)
    pl.semaphore_wait(barrier, n_sp - 1 + n_tp - 1)

    def spread(at, recv, far_sem, near_sem, s):
        for j in range(1, n_y):
            share(at, recv, s, q, far_sem.at[s, j], far(j)).start()
        share(at, recv, s, q, near_sem.at[s, 0], sibling).start()

    def relay(at, recv, near_sem, s):
        for j in range(1, n_y):
            t = behind(j)
            arrived(at, recv, s, t)
            share(at, recv, s, t, near_sem.at[s, j], sibling).start()

    def collect(at, recv, s):
        for j in range(n_y):
            arrived(at, recv, s, 2 * lax.rem(y + n_y - j, n_y) + (1 - core))

    def drain(at, recv, far_sem, near_sem, s):
        for j in range(1, n_y):
            share(at, recv, s, q, far_sem.at[s, j], far(j)).wait_send()
        share(at, recv, s, q, near_sem.at[s, 0], sibling).wait_send()
        for j in range(1, n_y):
            share(at, recv, s, behind(j), near_sem.at[s, j], sibling).wait_send()

    for o in range(1, n_tp):
        tell(o).start()
    for o in range(1, n_tp):
        t = lax.rem(q + o, n_tp)
        pltpu.make_async_copy(stats.at[t], stats.at[t], stat_recv.at[t]).wait()
    one = stats[0, 0:1]
    two = stats[0, 1:2]
    for t in range(1, n_tp):
        one = one + stats[t, 0:1]
        two = two + stats[t, 1:2]
    channels = proj.shape[0]
    mean = one / channels
    var = two / channels - mean * mean
    normed = (filtered[...] - mean) * lax.rsqrt(var + 1e-05) * gain[...]
    act[q] = (normed / (1.0 + jnp.exp(-normed))).astype(act.dtype)
    spread(act_at, act_recv, act_far, act_near, 0)
    relay(act_at, act_recv, act_near, 0)
    collect(act_at, act_recv, 0)
    depth = act.shape[1]
    sums = resid[...].astype(jnp.float32)
    for t in range(n_tp):
        sums = sums + lax.dot_general(
            act[t],
            proj[t * depth : (t + 1) * depth],
            (((0,), (0,)), ((), ())),
            preferred_element_type=jnp.float32,
        )
    mixed[...] = sums.astype(mixed.dtype)

    @pl.loop(0, n_sp)
    def _(k):
        to = target(k)
        place = (to * capacity + lax.broadcasted_iota(jnp.int32, (capacity, tokens), 0)).astype(
            jnp.float32
        )
        picks = jnp.zeros((capacity, tokens), jnp.float32)
        for r in range(top):
            picks = picks + jnp.where(place == slot_rows[r], 1.0, 0.0)
        outgoing[to] = jnp.dot(
            picks.astype(mixed.dtype), mixed[...], preferred_element_type=jnp.float32
        ).astype(outgoing.dtype)

        @pl.when(k > 0)
        def _():
            dispatch(k).start()

    total[...] = jnp.zeros_like(total)
    own_in = pltpu.make_async_copy(outgoing.at[e], rows_at(e, q), own_sem.at[0])
    own_in.start()

    def combine(x):
        place = (x * capacity + lax.broadcasted_iota(jnp.int32, (tokens, capacity), 1)).astype(
            jnp.float32
        )
        for r in range(top):
            picks = jnp.where(place == slots[:, r : r + 1], 1.0, 0.0).astype(mixed.dtype)
            got = jnp.dot(picks, returned[x], preferred_element_type=jnp.float32)
            total[...] += route[:, r : r + 1] * got

    tile = min(256, ff_local)
    out_tile = min(256, width)

    def up_step(s):
        @pl.loop(0, ff_local // tile)
        def _(i):
            at = pl.ds(pl.multiple_of(i * tile, tile), tile)
            g = jnp.dot(rows[s], gate_v[:, at], preferred_element_type=jnp.float32)
            u = jnp.dot(rows[s], up_v[:, at], preferred_element_type=jnp.float32)
            h = (g / (1.0 + jnp.exp(-g)) * u).astype(hidden.dtype)
            hidden[s, :, pl.ds(pl.multiple_of(q * ff_local + i * tile, tile), tile)] = h

    def down_step(s):
        @pl.loop(0, width // out_tile)
        def _(i):
            at = pl.ds(pl.multiple_of(i * out_tile, out_tile), out_tile)
            o = jnp.dot(hidden[s], down_v[:, at], preferred_element_type=jnp.float32)
            results[s, :, at] = o.astype(results.dtype)

    @pl.loop(0, n_sp + 4)
    def _(i):
        @pl.when(i < n_sp)
        def _():
            @pl.when(i == 0)
            def _():
                own_in.wait()

            @pl.when(i > 0)
            def _():
                arrived(rows_at, rows_recv, source(i), q)

            spread(rows_at, rows_recv, rows_far, rows_near, source(i))

        @pl.when((i >= 1) & (i < n_sp + 1))
        def _():
            relay(rows_at, rows_recv, rows_near, source(i - 1))

        @pl.when((i >= 2) & (i < n_sp + 2))
        def _():
            s = source(i - 2)
            collect(rows_at, rows_recv, s)

            @pl.when(i == 2)
            def _():
                for load in loads:
                    load.wait()

            up_step(s)
            spread(hidden_at, hid_recv, hid_far, hid_near, s)

        @pl.when((i >= 3) & (i < n_sp + 3))
        def _():
            relay(hidden_at, hid_recv, hid_near, source(i - 3))

        @pl.when(i >= 4)
        def _():
            s = source(i - 4)
            collect(hidden_at, hid_recv, s)
            down_step(s)

            @pl.when(i == 4)
            def _():
                pltpu.make_async_copy(results.at[e], returned.at[e], own_sem.at[1]).start()

            @pl.when(i > 4)
            def _():
                give_back(i - 4).start()

    pltpu.make_async_copy(results.at[e], returned.at[e], own_sem.at[1]).wait()
    combine(e)

    @pl.loop(1, n_sp)
    def _(k):
        x = target(k)
        pltpu.make_async_copy(returned.at[x], returned.at[x], ret_recv.at[x]).wait()
        combine(x)

    out[...] = (mixed[...].astype(jnp.float32) + total[...]).astype(out.dtype)

    for o in range(1, n_tp):
        tell(o).wait_send()
    drain(act_at, act_recv, act_far, act_near, 0)

    @pl.loop(0, n_sp)
    def _(s):
        drain(rows_at, rows_recv, rows_far, rows_near, s)
        drain(hidden_at, hid_recv, hid_far, hid_near, s)

    @pl.loop(1, n_sp)
    def _(k):
        dispatch(k).wait_send()
        give_back(k).wait_send()


def run_layer(filtered, gain, proj, resid, id_rows, id_cols, logits, prob, w_gate, w_up, w_down):
    n_sp, n_tp = lax.axis_size("sp"), lax.axis_size("tp")
    n_y = n_tp // 2
    tokens, width = resid.shape
    capacity = 4 * tokens // n_sp
    ff_local = w_gate.shape[2]
    dma = pltpu.SemaphoreType.DMA
    vmem = pl.BlockSpec(memory_space=pltpu.VMEM)
    return pl.pallas_call(
        functools.partial(expert_kernel, n_sp, n_tp),
        out_shape=jax.ShapeDtypeStruct(resid.shape, resid.dtype),
        in_specs=[vmem] * 8 + [pl.BlockSpec(memory_space=pl.ANY)] * 3,
        out_specs=vmem,
        scratch_shapes=[
            pltpu.VMEM((n_tp, 8, tokens), jnp.float32),
            pltpu.VMEM((n_tp,) + filtered.shape, jnp.bfloat16),
            pltpu.VMEM((tokens, width), jnp.bfloat16),
            pltpu.VMEM((tokens, id_cols.shape[1]), jnp.float32),
            pltpu.VMEM((tokens, id_cols.shape[1]), jnp.float32),
            pltpu.VMEM((tokens, width), jnp.float32),
            pltpu.VMEM((n_sp, capacity, width), jnp.bfloat16),
            pltpu.VMEM((n_sp, capacity, width * n_tp), jnp.bfloat16),
            pltpu.VMEM((n_sp, capacity, ff_local * n_tp), jnp.bfloat16),
            pltpu.VMEM((n_sp, capacity, width), jnp.bfloat16),
            pltpu.VMEM((n_sp, capacity, width), jnp.bfloat16),
            pltpu.VMEM(w_gate.shape[1:], jnp.bfloat16),
            pltpu.VMEM(w_up.shape[1:], jnp.bfloat16),
            pltpu.VMEM(w_down.shape[1:], jnp.bfloat16),
            dma((3,)),
            dma((2,)),
            dma((n_tp,)),
            dma((n_tp,)),
            dma((1, n_tp)),
            dma((1, n_y)),
            dma((1, n_y)),
            dma((n_sp,)),
            dma((n_sp, n_tp)),
            dma((n_sp, n_y)),
            dma((n_sp, n_y)),
            dma((n_sp, n_tp)),
            dma((n_sp, n_y)),
            dma((n_sp, n_y)),
            dma((n_sp,)),
            dma((n_sp,)),
        ],
        compiler_params=pltpu.CompilerParams(
            collective_id=0, has_side_effects=True, vmem_limit_bytes=52 * 1024 * 1024
        ),
    )(filtered, gain, proj, resid, id_rows, id_cols, logits, prob, w_gate, w_up, w_down)


def from_behind(block, axis, distance):
    devices = range(lax.axis_size(axis))
    route = [(i - distance, i) for i in devices if i - distance in devices]
    return lax.ppermute(block, axis, route)


def per_device(
    glu_value,
    glu_gate,
    conv_taps,
    norm_gain,
    out_proj,
    resid,
    expert_ids,
    route_logits,
    group_prob,
    w_gate,
    w_up,
    w_down,
):
    local_tokens = glu_value.shape[1]
    tap_count = conv_taps.shape[1]
    gated = (glu_value.astype(jnp.float32) * jax.nn.sigmoid(glu_gate.astype(jnp.float32))).astype(
        jnp.bfloat16
    )
    history = from_behind(gated[:, local_tokens - (tap_count - 1) :], "sp", 1)
    padded = jnp.concatenate([history, gated], axis=1).astype(jnp.float32)
    filtered = jnp.zeros(gated.shape, jnp.float32)
    for offset in range(tap_count):
        filtered = (
            filtered + conv_taps[:, offset : offset + 1] * padded[:, offset : offset + local_tokens]
        )
    return run_layer(
        filtered,
        norm_gain[:, None],
        out_proj,
        resid,
        expert_ids.T,
        expert_ids,
        route_logits,
        group_prob[:, None],
        w_gate,
        w_up,
        w_down,
    )


def solution(mesh):
    return jax.shard_map(
        per_device,
        mesh=mesh,
        in_specs=(
            P("tp", "sp"),
            P("tp", "sp"),
            P("tp", None),
            P("tp"),
            P(None, "tp"),
            P("sp", "tp"),
            P("sp", None),
            P("sp", None),
            P("sp"),
            P("sp", None, "tp"),
            P("sp", None, "tp"),
            P("sp", None, "tp"),
        ),
        out_specs=P("sp", "tp"),
        check_vma=False,
    )
```
